32 devices in a mesh: rep: 2 (over core), fs: 8 (over z, y), tp: 2 (over x).
Axes of the slice: x: 2, y: 2, z: 4, core: 2. Of those that a mesh axis runs over, the one named last changes fastest.
Arguments:
- tokens: bfloat16 [16, 768, 2048], P(('rep', 'fs')), may hold values from -6 to 6
- mixer_gain: float32 [2048], replicated, may hold values from 0.1 to 1.9
- value_weight: float32 [2048, 4, 512], P('fs', None, 'tp'), may hold values from -0.125 to 0.125
- value_scale: float32 [4, 512], P(None, 'tp'), may hold values from 0.5 to 2
- gate_weight: float32 [2048, 4, 512], P('fs', None, 'tp'), may hold values from -0.125 to 0.125
- gate_scale: float32 [4, 512], P(None, 'tp'), may hold values from 0.5 to 2
- pool_weight: float32 [4, 512, 512], P(None, 'fs', 'tp'), may hold values from -0.25 to 0.25
- pool_scale: float32 [4, 512], P(None, 'tp'), may hold values from 0.5 to 2
- channel_gain: float32 [2048], replicated, may hold values from 0.1 to 1.9
- up_weight: float32 [2048, 4096], P('fs', 'tp'), may hold values from -0.125 to 0.125
- up_scale: float32 [4096], P('tp'), may hold values from 0.5 to 2
- down_weight: float32 [4096, 2048], P('tp', 'fs'), may hold values from -0.09375 to 0.09375
- down_scale: float32 [2048], P('fs'), may hold values from 0.5 to 2
Outputs:
- layer_out: bfloat16 [16, 768, 2048], P(('rep', 'fs'), 'tp')
The draws below stay inside these ranges and needn't reach their ends.
All inputs are finite; a program needn't handle non-finite values.
Results may differ from the reference program's by a relative error of at most 0.015.
Values may be sent and summed in bfloat16 or wider, within the bound.
No kernel may reach another device: no remote copies, remote signals or barrier semaphores. Data moves between devices by JAX's collectives and lax.ppermute only.
A program may use at most 64 MiB of HBM per device.

```python
import math
import jax
import jax.numpy as jnp
from jax import lax

D = 2048
GROUPS = 4
GROUP_WIDTH = 512
FF = 4096
SEQ_LEN = 768
SEQS = 16
N_TP = 2


def levels(rng, dims, pieces, low, high):
    loudness, own = 1.0, jax.random.fold_in(rng, 6)
    for dim, parts in pieces:
        steps = jnp.exp(jax.random.uniform(jax.random.fold_in(own, dim), (parts,), jnp.float32, low / len(pieces), high / len(pieces)))
        loudness = loudness * jnp.repeat(steps, dims[dim] // parts).reshape([-1 if axis == dim else 1 for axis in range(len(dims))])
    return loudness


def normal_values(own_key, dims, scale, limit, shards=(), dtype=jnp.bfloat16):
    loudness = levels(own_key, dims, shards, -0.22, 0.18) if shards else 1.0
    values = jax.random.normal(own_key, dims, jnp.float32) * scale * loudness
    return jnp.minimum(jnp.maximum(values, -limit), limit).astype(dtype)


def setup_inputs(seed: int = 0) -> dict:
    seeds = jax.random.split(jax.random.key(seed), 14)
    tokens = normal_values(seeds[0], (SEQS, SEQ_LEN, D), 1.0, 6.0, ((0, 16),))
    mixer_gain = jnp.clip(1.0 + 0.18 * jax.random.normal(seeds[1], (D,), jnp.float32), 0.1, 1.9)
    value_weight = normal_values(seeds[2], (D, GROUPS, GROUP_WIDTH), D ** -0.5, 0.125, ((0, 8), (2, 2)), jnp.float32)
    value_scale = jnp.clip(jnp.exp(math.log(2.0) - 1.3862944 * jax.random.uniform(seeds[3], (GROUPS, GROUP_WIDTH), jnp.float32) ** levels(seeds[3], (GROUPS, GROUP_WIDTH), ((1, 2),), -0.2, 0.2)), 0.5, 2.0)
    gate_weight = normal_values(seeds[4], (D, GROUPS, GROUP_WIDTH), D ** -0.5, 0.125, ((0, 8), (2, 2)), jnp.float32)
    gate_scale = jnp.clip(jnp.exp(math.log(2.0) - 1.3862944 * jax.random.uniform(seeds[5], (GROUPS, GROUP_WIDTH), jnp.float32) ** levels(seeds[5], (GROUPS, GROUP_WIDTH), ((1, 2),), -0.2, 0.2)), 0.5, 2.0)
    pool_weight = normal_values(seeds[6], (GROUPS, GROUP_WIDTH, GROUP_WIDTH), GROUP_WIDTH ** -0.5, 0.25, ((1, 8), (2, 2)), jnp.float32)
    pool_scale = jnp.clip(jnp.exp(math.log(2.0) - 1.3862944 * jax.random.uniform(seeds[7], (GROUPS, GROUP_WIDTH), jnp.float32) ** levels(seeds[7], (GROUPS, GROUP_WIDTH), ((1, 2),), -0.2, 0.2)), 0.5, 2.0)
    channel_gain = jnp.clip(1.0 + 0.18 * jax.random.normal(seeds[8], (D,), jnp.float32), 0.1, 1.9)
    up_weight = normal_values(seeds[9], (D, FF), D ** -0.5, 0.125, ((0, 8), (1, 2)), jnp.float32)
    up_scale = jnp.clip(jnp.exp(math.log(2.0) - 1.3862944 * jax.random.uniform(seeds[10], (FF,), jnp.float32) ** levels(seeds[10], (FF,), ((0, 2),), -0.2, 0.2)), 0.5, 2.0)
    down_weight = normal_values(seeds[11], (FF, D), FF ** -0.5, 0.09375, ((0, 2), (1, 8)), jnp.float32)
    down_scale = jnp.clip(jnp.exp(math.log(2.0) - 1.3862944 * jax.random.uniform(seeds[12], (D,), jnp.float32) ** levels(seeds[12], (D,), ((0, 8),), -0.2, 0.2)), 0.5, 2.0)
    return dict(tokens=tokens, mixer_gain=mixer_gain, value_weight=value_weight, value_scale=value_scale, gate_weight=gate_weight, gate_scale=gate_scale, pool_weight=pool_weight, pool_scale=pool_scale, channel_gain=channel_gain, up_weight=up_weight, up_scale=up_scale, down_weight=down_weight, down_scale=down_scale)


def norm_rows(values, gain):
    floats = values.astype(jnp.float32)
    return floats * lax.rsqrt(lax.optimization_barrier(jnp.mean(floats * floats, axis=-1, keepdims=True)) + 1e-06) * gain

def pool_excess(value):
    floats = value.astype(jnp.float32)
    seq_length = floats.shape[1]
    running = floats
    results = []
    for group in range(floats.shape[2]):
        span = 2 ** group
        shifted = jnp.pad(running, ((0, 0), (span, 0), (0, 0), (0, 0)))[:, :seq_length]
        running = running + shifted
        counts = jnp.minimum(jnp.arange(1, seq_length + 1), 2 * span).astype(jnp.float32)
        results.append(running[:, :, group, :] / counts[None, :, None] - floats[:, :, group, :])
    return jnp.stack(results, axis=2)

def rounded(values):
    return lax.optimization_barrier(values.astype(jnp.bfloat16)).astype(jnp.float32)

def reference(tokens, mixer_gain, value_weight, value_scale, gate_weight, gate_scale, pool_weight, pool_scale, channel_gain, up_weight, up_scale, down_weight, down_scale):
    seq_count, seq_length, model_width = tokens.shape
    row_count = seq_count * seq_length
    normed = norm_rows(tokens, mixer_gain).astype(jnp.bfloat16).reshape(row_count, model_width)
    value = jnp.dot(normed, value_weight.astype(jnp.bfloat16).reshape(model_width, -1), preferred_element_type=jnp.float32)
    value = (value * value_scale.reshape(-1)).astype(jnp.bfloat16).reshape(seq_count, seq_length, GROUPS, GROUP_WIDTH)
    gate = jnp.dot(normed, gate_weight.astype(jnp.bfloat16).reshape(model_width, -1), preferred_element_type=jnp.float32)
    gate = (gate * gate_scale.reshape(-1)).reshape(seq_count, seq_length, GROUPS, GROUP_WIDTH)
    excess = pool_excess(value).astype(jnp.bfloat16)
    pooled = jnp.einsum('slgc,gce->slge', excess.astype(jnp.float32), pool_weight.astype(jnp.bfloat16).astype(jnp.float32)) * pool_scale
    merged = (jax.nn.sigmoid(gate) * pooled).astype(jnp.bfloat16)
    middle = tokens.reshape(row_count, model_width).astype(jnp.float32) + merged.reshape(row_count, model_width).astype(jnp.float32)
    normed_two = norm_rows(middle, channel_gain).astype(jnp.bfloat16)
    upward = jnp.dot(normed_two, up_weight.astype(jnp.bfloat16), preferred_element_type=jnp.float32) * up_scale
    hidden = jnp.square(jax.nn.relu(upward)).astype(jnp.bfloat16)
    down_matrix = down_weight.astype(jnp.bfloat16)
    hidden_block = FF // N_TP
    summed = jnp.zeros((row_count, model_width), jnp.float32)
    for member in range(N_TP):
        part = hidden[:, member * hidden_block:(member + 1) * hidden_block]
        rows_part = down_matrix[member * hidden_block:(member + 1) * hidden_block]
        summed = summed + rounded(jnp.dot(part, rows_part, preferred_element_type=jnp.float32) * down_scale)
    return (middle + summed).astype(jnp.bfloat16).reshape(seq_count, seq_length, model_width)
```

```python
import functools

import jax
import jax.numpy as jnp
from jax import lax
from jax.experimental import pallas as pl
from jax.experimental.pallas import tpu as pltpu
from jax.sharding import PartitionSpec as P

EPS = 1e-06
BF16 = jnp.bfloat16
F32 = jnp.float32


def norm_rows(values, gain):
    floats = values.astype(F32)
    return floats * lax.rsqrt(jnp.mean(floats * floats, axis=-1, keepdims=True) + EPS) * gain


def pool_excess(value):
    floats = value.astype(F32)
    seq_length = floats.shape[1]
    running = floats
    results = []
    for group in range(floats.shape[2]):
        span = 2**group
        shifted = jnp.pad(running, ((0, 0), (span, 0), (0, 0), (0, 0)))[:, :seq_length]
        running = running + shifted
        counts = jnp.minimum(jnp.arange(1, seq_length + 1), 2 * span).astype(F32)
        results.append(running[:, :, group, :] / counts[None, :, None] - floats[:, :, group, :])
    return jnp.stack(results, axis=2)


def general(
    tokens,
    mixer_gain,
    value_weight,
    value_scale,
    gate_weight,
    gate_scale,
    pool_weight,
    pool_scale,
    channel_gain,
    up_weight,
    up_scale,
    down_weight,
    down_scale,
):
    seq_count, seq_length, model_width = tokens.shape
    shares = lax.axis_size("tp")
    member = lax.axis_index("tp")
    kept_rows = seq_length // shares
    row_count = seq_count * seq_length
    group_count, local_width = value_scale.shape
    value_full = lax.all_gather(value_weight.astype(BF16), "fs", axis=0, tiled=True)
    gate_full = lax.all_gather(gate_weight.astype(BF16), "fs", axis=0, tiled=True)
    pool_full = lax.all_gather(pool_weight.astype(BF16), "fs", axis=1, tiled=True)
    down_scales = lax.all_gather(down_scale, "fs", axis=0, tiled=True)
    normed = norm_rows(tokens, mixer_gain).astype(BF16).reshape(row_count, model_width)
    value = jnp.dot(normed, value_full.reshape(model_width, -1), preferred_element_type=F32)
    value = (value * value_scale.reshape(-1)).astype(BF16)
    value = value.reshape(seq_count, seq_length, group_count, local_width)
    gating = jnp.dot(normed, gate_full.reshape(model_width, -1), preferred_element_type=F32)
    gating = gating * gate_scale.reshape(-1)
    gating = gating.reshape(seq_count, seq_length, group_count, local_width)
    excess = pool_excess(value).astype(BF16)
    pooled = jnp.einsum(
        "slgc,gce->slge",
        lax.all_gather(excess, "tp", axis=3, tiled=True),
        pool_full,
        preferred_element_type=F32,
    )
    merged = (jax.nn.sigmoid(gating) * (pooled * pool_scale)).astype(BF16)
    merged_own = lax.all_to_all(merged, "tp", split_axis=1, concat_axis=3, tiled=True)
    own_rows = lax.dynamic_slice_in_dim(tokens, member * kept_rows, kept_rows, 1)
    middle = own_rows.reshape(seq_count * kept_rows, model_width).astype(F32)
    middle = middle + merged_own.reshape(seq_count * kept_rows, model_width).astype(F32)
    normed_two = norm_rows(middle, channel_gain).astype(BF16)
    up_full = lax.all_gather(up_weight.astype(BF16), "fs", axis=0, tiled=True)
    down_full = lax.all_gather(down_weight.astype(BF16), "fs", axis=1, tiled=True)
    all_two = lax.all_gather(normed_two, "tp", axis=0, tiled=True)
    upward = jnp.dot(all_two, up_full, preferred_element_type=F32) * up_scale
    hidden = jnp.square(jax.nn.relu(upward)).astype(BF16)
    partial = jnp.dot(hidden, down_full, preferred_element_type=F32) * down_scales
    summed = lax.psum_scatter(partial.astype(BF16), "tp", scatter_dimension=0, tiled=True)
    out = middle + summed.astype(F32)
    return out.astype(BF16).reshape(seq_count, kept_rows, model_width)


def dot(a, b):
    return jnp.dot(a, b, preferred_element_type=F32)


def ring_order(count):
    return list(range(0, count, 2)) + list(range(1, count, 2))[::-1]


def mixer_kernel(depth, rows, tile, idx, x_hbm, *refs):
    blocks = len(refs) - 6
    srcs, (out, xv, wv, acc, pv, sem) = refs[:blocks], refs[blocks:]
    width = out.shape[1]
    part = (wv.shape[1] - depth) * 2

    copies = []
    for k in range(blocks):
        cols = pl.ds(pl.multiple_of(idx[k] * depth, depth), depth)
        copies.append(
            (
                pltpu.make_async_copy(srcs[k], wv.at[k], sem.at[0, k]),
                pltpu.make_async_copy(x_hbm.at[:, cols], xv.at[k], sem.at[1, k]),
            )
        )
    for pair in copies:
        for copy in pair:
            copy.start()
    window = idx[blocks]
    for k in range(blocks):
        for copy in copies[k]:
            copy.wait()
        base = pl.multiple_of(idx[k] * part, part)
        half = part // 2
        pv[pl.ds(base, half), :] = wv[k, depth:, :width]
        pv[pl.ds(base + half, half), :] = wv[k, depth:, width:]

    def product(m, carry):
        at = pl.ds(pl.multiple_of(m * tile, tile), tile)
        total = dot(xv[0, at, :], wv[0, :depth, :])
        for k in range(1, blocks):
            total = total + dot(xv[k, at, :], wv[k, :depth, :])
        acc[at, :] = total
        return carry

    lax.fori_loop(0, rows // tile, product, 0)

    t = lax.broadcasted_iota(jnp.int32, (tile, tile), 0)
    s = lax.broadcasted_iota(jnp.int32, (tile, tile), 1)
    here = jnp.where((s <= t) & (s > t - window), 1.0, 0.0).astype(BF16)
    back = jnp.where(s - tile > t - window, 1.0, 0.0).astype(BF16)
    for m in range(rows // tile):
        at = pl.ds(m * tile, tile)
        value = acc[at, :width].astype(BF16)
        running = dot(here, value)
        if m:
            before = acc[pl.ds((m - 1) * tile, tile), :width].astype(BF16)
            running = running + dot(back, before)
        place = lax.broadcasted_iota(jnp.int32, (tile, 1), 0) + m * tile
        counts = jnp.minimum(place + 1, window).astype(F32)
        excess = (running / counts - value.astype(F32)).astype(BF16)
        pooled = dot(excess, pv[...])
        out[at, :] = (jax.nn.sigmoid(acc[at, width:]) * pooled).astype(BF16)


def mixer(idx, x, blocks, part):
    rows = x.shape[0]
    depth = blocks[0].shape[0] - part // 2
    width = blocks[0].shape[1] // 2
    count = len(blocks)
    tile = 256 if rows % 256 == 0 else rows
    anywhere = pl.BlockSpec(memory_space=pl.ANY)
    flops = 2 * rows * (count * depth * 2 * width + 2 * tile * width + width * width)
    return pl.pallas_call(
        functools.partial(mixer_kernel, depth, rows, tile),
        out_shape=jax.ShapeDtypeStruct((rows, width), BF16),
        in_specs=[pl.BlockSpec(memory_space=pltpu.SMEM)] + [anywhere] * (count + 1),
        out_specs=pl.BlockSpec(memory_space=pltpu.VMEM),
        scratch_shapes=[
            pltpu.VMEM((count, rows, depth), BF16),
            pltpu.VMEM((count,) + blocks[0].shape, BF16),
            pltpu.VMEM((rows, 2 * width), F32),
            pltpu.VMEM((count * part, width), BF16),
            pltpu.SemaphoreType.DMA((2, count)),
        ],
        cost_estimate=pl.CostEstimate(
            flops=flops, bytes_accessed=2 * (x.size + count * blocks[0].size), transcendentals=0
        ),
        compiler_params=pltpu.CompilerParams(vmem_limit_bytes=40 * 2**20),
        name="mixer",
    )(idx, x, *blocks)


def middle_kernel(gain, place, tokens, m0, m1, m2, m3, normed, middle):
    width = m0.shape[1]
    total = jnp.zeros((tokens.shape[0], 1), F32)
    for k, part in enumerate((m0, m1, m2, m3)):
        cols = pl.ds(pl.multiple_of(place[k] * width, width), width)
        values = tokens[:, cols].astype(F32) + part[...].astype(F32)
        middle[:, cols] = values
        total = total + jnp.sum(values * values, axis=1, keepdims=True)
    scale = lax.rsqrt(total / tokens.shape[1] + EPS)
    normed[...] = (middle[...] * scale * gain[...]).astype(BF16)


def middle_norm(place, tokens, parts, gain):
    rows, model = tokens.shape
    tile = 128 if rows % 128 == 0 else rows
    width = parts[0].shape[1]
    at = lambda i: (i, 0)
    return pl.pallas_call(
        lambda place, gain, *refs: middle_kernel(gain, place, *refs),
        grid=(rows // tile,),
        out_shape=[
            jax.ShapeDtypeStruct((rows, model), BF16),
            jax.ShapeDtypeStruct((rows, model), F32),
        ],
        in_specs=[
            pl.BlockSpec(memory_space=pltpu.SMEM),
            pl.BlockSpec((1, model), lambda i: (0, 0)),
            pl.BlockSpec((tile, model), at),
        ]
        + [pl.BlockSpec((tile, width), at)] * 4,
        out_specs=[pl.BlockSpec((tile, model), at)] * 2,
        cost_estimate=pl.CostEstimate(
            flops=8 * rows * model, bytes_accessed=10 * rows * model, transcendentals=0
        ),
        name="middle",
    )(place, gain.reshape(1, model), tokens, *parts)


def up_kernel(depth, rows, tile, idx, x_hbm, *refs):
    blocks = len(refs) - 4
    srcs, (out, xv, wv, sem) = refs[:blocks], refs[blocks:]
    copies = []
    for k in range(blocks):
        cols = pl.ds(pl.multiple_of(idx[k] * depth, depth), depth)
        copies.append(
            (
                pltpu.make_async_copy(srcs[k], wv.at[k], sem.at[0, k]),
                pltpu.make_async_copy(x_hbm.at[:, cols], xv.at[k], sem.at[1, k]),
            )
        )
    for pair in copies:
        for copy in pair:
            copy.start()
    for pair in copies:
        for copy in pair:
            copy.wait()

    def product(m, carry):
        at = pl.ds(pl.multiple_of(m * tile, tile), tile)
        total = dot(xv[0, at, :], wv[0])
        for k in range(1, blocks):
            total = total + dot(xv[k, at, :], wv[k])
        total = jnp.maximum(total, 0.0)
        out[at, :] = (total * total).astype(BF16)
        return carry

    lax.fori_loop(0, rows // tile, product, 0)


def upward(idx, x, blocks):
    rows = x.shape[0]
    depth, width = blocks[0].shape
    count = len(blocks)
    tile = 256 if rows % 256 == 0 else rows
    anywhere = pl.BlockSpec(memory_space=pl.ANY)
    return pl.pallas_call(
        functools.partial(up_kernel, depth, rows, tile),
        out_shape=jax.ShapeDtypeStruct((rows, width), BF16),
        in_specs=[pl.BlockSpec(memory_space=pltpu.SMEM)] + [anywhere] * (count + 1),
        out_specs=pl.BlockSpec(memory_space=pltpu.VMEM),
        scratch_shapes=[
            pltpu.VMEM((count, rows, depth), BF16),
            pltpu.VMEM((count, depth, width), BF16),
            pltpu.SemaphoreType.DMA((2, count)),
        ],
        cost_estimate=pl.CostEstimate(
            flops=2 * rows * count * depth * width,
            bytes_accessed=2 * (x.size + count * depth * width),
            transcendentals=0,
        ),
        compiler_params=pltpu.CompilerParams(vmem_limit_bytes=40 * 2**20),
        name="upward",
    )(idx, x, *blocks)


def down_kernel(kept, member, h0, h1, *refs):
    count = (len(refs) - 2) // 2
    own, other = refs[:count], refs[count : 2 * count]
    keep, send = refs[2 * count :]
    width = own[0].shape[1]
    for out, who in ((send, 1 - member[0]), (keep, member[0])):
        at = pl.ds(pl.multiple_of(who * kept, kept), kept)
        for k in range(count):
            total = dot(h0[at, :], own[k][...]) + dot(h1[at, :], other[k][...])
            out[:, k * width : (k + 1) * width] = total.astype(BF16)


def down(member, h0, h1, own, other, kept):
    count = len(own)
    depth, width = own[0].shape
    return pl.pallas_call(
        functools.partial(down_kernel, kept),
        out_shape=[jax.ShapeDtypeStruct((kept, count * width), BF16)] * 2,
        in_specs=[pl.BlockSpec(memory_space=pltpu.SMEM)]
        + [pl.BlockSpec(memory_space=pltpu.VMEM)] * (2 + 2 * count),
        out_specs=[pl.BlockSpec(memory_space=pltpu.VMEM)] * 2,
        cost_estimate=pl.CostEstimate(
            flops=4 * h0.size * count * width,
            bytes_accessed=4 * (h0.size + count * own[0].size),
            transcendentals=0,
        ),
        compiler_params=pltpu.CompilerParams(vmem_limit_bytes=40 * 2**20),
        name="down",
    )(member, h0, h1, *own, *other)


def final_kernel(group, idx, middle, *refs):
    count = (len(refs) - 1) // 2
    keeps, gots, out = refs[:count], refs[count : 2 * count], refs[-1]
    width = keeps[0].shape[1] // group
    for j in range(count):
        for k in range(group):
            part = slice(k * width, (k + 1) * width)
            cols = pl.ds(pl.multiple_of(idx[j * group + k] * width, width), width)
            summed = keeps[j][:, part].astype(F32) + gots[j][:, part].astype(F32)
            out[:, cols] = (middle[:, cols] + summed).astype(BF16)


def final(idx, member, middle, keeps, gots, group):
    rows, model = middle.shape
    kept = keeps[0].shape[0]
    tile = 128 if kept % 128 == 0 else kept
    steps = kept // tile
    at = lambda i, *s: (i, 0)
    return pl.pallas_call(
        lambda idx, member, *refs: final_kernel(group, idx, *refs),
        grid_spec=pltpu.PrefetchScalarGridSpec(
            num_scalar_prefetch=2,
            grid=(steps,),
            in_specs=[pl.BlockSpec((tile, model), lambda i, idx, mem: (mem[0] * steps + i, 0))]
            + [pl.BlockSpec((tile, keeps[0].shape[1]), at)] * (2 * len(keeps)),
            out_specs=pl.BlockSpec((tile, model), at),
        ),
        out_shape=jax.ShapeDtypeStruct((kept, model), BF16),
        cost_estimate=pl.CostEstimate(
            flops=2 * kept * model, bytes_accessed=10 * kept * model, transcendentals=0
        ),
        name="final",
    )(idx, member, middle, *keeps, *gots)


def paired(
    tokens,
    mixer_gain,
    value_weight,
    value_scale,
    gate_weight,
    gate_scale,
    pool_weight,
    pool_scale,
    channel_gain,
    up_weight,
    up_scale,
    down_weight,
    down_scale,
):
    _, rows, model = tokens.shape
    tokens = tokens.reshape(rows, model)
    fs = lax.axis_size("fs")
    line = fs // 2
    t, r, f = lax.axis_index("tp"), lax.axis_index("rep"), lax.axis_index("fs")
    kept = rows // 2
    depth = value_weight.shape[0]
    half_width = value_weight.shape[2]
    part = pool_weight.shape[1]

    order = ring_order(line)
    place = {z: p for p, z in enumerate(order)}
    swap = [(0, 1), (1, 0)]
    side = [(z * 2 + y, z * 2 + 1 - y) for z in range(line) for y in range(2)]
    step = [
        (z * 2 + y, order[(place[z] + 1) % line] * 2 + y) for z in range(line) for y in range(2)
    ]
    across = lambda v: lax.ppermute(v, "tp", swap)
    core = lambda v: lax.ppermute(v, "rep", swap)
    beside = lambda v: lax.ppermute(v, "fs", side)
    onward = lambda v: lax.ppermute(v, "fs", step)

    table = jnp.array(
        [[order[(place[z] - k) % line] for k in range(line)] for z in range(line)], jnp.int32
    )
    mine = table[f // 2] * 2
    blocks_at = jnp.concatenate([mine + f % 2, mine + 1 - f % 2])

    def gathered(block, by_side):
        own, other = [block], []
        for k in range(line):
            if k < line - 1 or by_side:
                other.append(beside(own[k]))
            else:
                other.append(onward(other[k - 1]))
            if k < line - 1:
                own.append(onward(own[k]))
        blocks = own + other
        return blocks, [core(b) for b in blocks]

    def group_half(group):
        pick = lambda a, axis: lax.dynamic_index_in_dim(a, group, axis, keepdims=False)
        value = pick(value_weight, 1) * pick(value_scale, 0)
        gate = pick(gate_weight, 1) * pick(gate_scale, 0)
        pool = pick(pool_weight, 0) * pick(pool_scale, 0)
        top = jnp.concatenate([value, gate], axis=1)
        low = jnp.concatenate([pool[: part // 2], pool[part // 2 :]], axis=1)
        return jnp.concatenate([top, low], axis=0).astype(BF16)

    got = across(group_half(2 * (1 - t) + r))
    own = group_half(2 * t + r)
    w = half_width
    first, second = jnp.where(t == 0, own, got), jnp.where(t == 0, got, own)
    mix_block = jnp.concatenate([first[:, :w], second[:, :w], first[:, w:], second[:, w:]], axis=1)

    up_width = up_weight.shape[1] // 2
    up_own = lax.dynamic_slice_in_dim(up_weight, r * up_width, up_width, 1)
    up_block = (up_own * lax.dynamic_slice_in_dim(up_scale, r * up_width, up_width, 0)).astype(BF16)
    down_depth = down_weight.shape[0] // 2
    down_block = lax.dynamic_slice_in_dim(down_weight, r * down_depth, down_depth, 0)
    down_block = (down_block * down_scale).astype(BF16)

    mix_own, mix_other = gathered(mix_block, False)
    up_mine, up_theirs = gathered(up_block, True)
    down_mine, down_theirs = gathered(down_block, False)

    normed = norm_rows(tokens, mixer_gain).astype(BF16)

    def group_index(group):
        return jnp.concatenate([blocks_at, jnp.left_shift(2, group).reshape(1).astype(jnp.int32)])

    merged_own = mixer(group_index(2 * t + r), normed, mix_own, part)
    from_own = across(merged_own)
    merged_other = mixer(group_index(2 * t + 1 - r), normed, mix_other, part)
    from_other = across(merged_other)

    groups = jnp.stack([2 * t + r, 2 * t + 1 - r, 2 * (1 - t) + r, 2 * (1 - t) + 1 - r])
    normed_two, middle = middle_norm(
        groups.astype(jnp.int32), tokens, (merged_own, merged_other, from_own, from_other), channel_gain
    )
    hidden_own = upward(blocks_at, normed_two, up_mine)
    hidden_other = upward(blocks_at, normed_two, up_theirs)

    member = t.reshape(1).astype(jnp.int32)
    keeps, gots, sequence = [], [], []
    for k in range(line):
        which = (k, line + k)
        keep, send = down(
            member,
            hidden_own,
            hidden_other,
            [down_mine[i] for i in which],
            [down_theirs[i] for i in which],
            kept,
        )
        keeps.append(keep)
        gots.append(across(send))
        sequence += which
    out = final(blocks_at[jnp.array(sequence)], member, middle, keeps, gots, 2)
    return out.reshape(1, kept, model)


def solution(mesh):
    sizes = dict(mesh.shape)

    def per_device(tokens, mixer_gain, value_weight, value_scale, *rest):
        fits = (
            sizes["rep"] == 2
            and sizes["tp"] == 2
            and sizes["fs"] % 4 == 0
            and tokens.shape[0] == 1
            and value_scale.shape[0] == 4
            and value_weight.shape[0] % 128 == 0
            and value_weight.shape[2] % 128 == 0
            and rest[2].shape[1] % 32 == 0
            and tokens.shape[1] % 256 == 0
        )
        return (paired if fits else general)(
            tokens, mixer_gain, value_weight, value_scale, *rest
        )

    return jax.shard_map(
        per_device,
        mesh=mesh,
        in_specs=(
            P(("rep", "fs"), None, None),
            P(),
            P("fs", None, "tp"),
            P(None, "tp"),
            P("fs", None, "tp"),
            P(None, "tp"),
            P(None, "fs", "tp"),
            P(None, "tp"),
            P(),
            P("fs", "tp"),
            P("tp"),
            P("tp", "fs"),
            P("fs"),
        ),
        out_specs=P(("rep", "fs"), "tp", None),
        check_vma=False,
    )
```

```python
import functools

import jax
import jax.numpy as jnp
import numpy as np
from jax import lax
from jax.experimental import pallas as pl
from jax.experimental.pallas import tpu as pltpu
from jax.sharding import PartitionSpec as P


EPS = 1e-06
BF16 = jnp.bfloat16
F32 = jnp.float32


def norm_rows(values, gain):
    floats = values.astype(F32)
    return floats * lax.rsqrt(jnp.mean(floats * floats, axis=-1, keepdims=True) + EPS) * gain


def pool_excess(value):
    floats = value.astype(F32)
    seq_length = floats.shape[1]
    running = floats
    results = []
    for group in range(floats.shape[2]):
        span = 2**group
        shifted = jnp.pad(running, ((0, 0), (span, 0), (0, 0), (0, 0)))[:, :seq_length]
        running = running + shifted
        counts = jnp.minimum(jnp.arange(1, seq_length + 1), 2 * span).astype(F32)
        results.append(running[:, :, group, :] / counts[None, :, None] - floats[:, :, group, :])
    return jnp.stack(results, axis=2)


def general(
    tokens,
    mixer_gain,
    value_weight,
    value_scale,
    gate_weight,
    gate_scale,
    pool_weight,
    pool_scale,
    channel_gain,
    up_weight,
    up_scale,
    down_weight,
    down_scale,
):
    seq_count, seq_length, model_width = tokens.shape
    shares = lax.axis_size("tp")
    member = lax.axis_index("tp")
    kept_rows = seq_length // shares
    row_count = seq_count * seq_length
    group_count, local_width = value_scale.shape
    value_full = lax.all_gather(value_weight.astype(BF16), "fs", axis=0, tiled=True)
    gate_full = lax.all_gather(gate_weight.astype(BF16), "fs", axis=0, tiled=True)
    pool_full = lax.all_gather(pool_weight.astype(BF16), "fs", axis=1, tiled=True)
    down_scales = lax.all_gather(down_scale, "fs", axis=0, tiled=True)
    normed = norm_rows(tokens, mixer_gain).astype(BF16).reshape(row_count, model_width)
    value = jnp.dot(normed, value_full.reshape(model_width, -1), preferred_element_type=F32)
    value = (value * value_scale.reshape(-1)).astype(BF16)
    value = value.reshape(seq_count, seq_length, group_count, local_width)
    gating = jnp.dot(normed, gate_full.reshape(model_width, -1), preferred_element_type=F32)
    gating = gating * gate_scale.reshape(-1)
    gating = gating.reshape(seq_count, seq_length, group_count, local_width)
    excess = pool_excess(value).astype(BF16)
    pooled = jnp.einsum(
        "slgc,gce->slge",
        lax.all_gather(excess, "tp", axis=3, tiled=True),
        pool_full,
        preferred_element_type=F32,
    )
    merged = (jax.nn.sigmoid(gating) * (pooled * pool_scale)).astype(BF16)
    merged_own = lax.all_to_all(merged, "tp", split_axis=1, concat_axis=3, tiled=True)
    own_rows = lax.dynamic_slice_in_dim(tokens, member * kept_rows, kept_rows, 1)
    middle = own_rows.reshape(seq_count * kept_rows, model_width).astype(F32)
    middle = middle + merged_own.reshape(seq_count * kept_rows, model_width).astype(F32)
    normed_two = norm_rows(middle, channel_gain).astype(BF16)
    up_full = lax.all_gather(up_weight.astype(BF16), "fs", axis=0, tiled=True)
    down_full = lax.all_gather(down_weight.astype(BF16), "fs", axis=1, tiled=True)
    all_two = lax.all_gather(normed_two, "tp", axis=0, tiled=True)
    upward = jnp.dot(all_two, up_full, preferred_element_type=F32) * up_scale
    hidden = jnp.square(jax.nn.relu(upward)).astype(BF16)
    partial = jnp.dot(hidden, down_full, preferred_element_type=F32) * down_scales
    summed = lax.psum_scatter(partial.astype(BF16), "tp", scatter_dimension=0, tiled=True)
    out = middle + summed.astype(F32)
    return out.astype(BF16).reshape(seq_count, kept_rows, model_width)


def dot(a, b):
    return jnp.dot(a, b, preferred_element_type=F32)


def ring_order(count):
    return list(range(0, count, 2)) + list(range(1, count, 2))[::-1]


def prep_kernel(at, value, gate, pool, scales, own, send, vals, low, sem):
    width = vals.shape[-1]
    depth, part = vals.shape[2], low.shape[1]
    copies = []
    for j in range(2):
        group = at[j]
        copies.append(
            [
                pltpu.make_async_copy(value.at[:, group, :], vals.at[j, 0], sem.at[j, 0]),
                pltpu.make_async_copy(gate.at[:, group, :], vals.at[j, 1], sem.at[j, 1]),
                pltpu.make_async_copy(pool.at[group], low.at[j], sem.at[j, 2]),
            ]
        )
        for copy in copies[j]:
            copy.start()
    for j, out in enumerate((own, send)):
        for copy in copies[j]:
            copy.wait()
        group = at[j]
        for i in range(2):
            scale = scales[i, pl.ds(group, 1), :]
            out[:depth, i * width : (i + 1) * width] = (vals[j, i] * scale).astype(BF16)
        scaled = low[j] * scales[2, pl.ds(group, 1), :]
        for i in range(2):
            rows = slice(i * part // 2, (i + 1) * part // 2)
            out[depth:, i * width : (i + 1) * width] = scaled[rows, :].astype(BF16)


def prepare(at, value, gate, pool, scales):
    depth, _, width = value.shape
    part = pool.shape[1]
    anywhere = pl.BlockSpec(memory_space=pl.ANY)
    vmem = pl.BlockSpec(memory_space=pltpu.VMEM)
    return pl.pallas_call(
        prep_kernel,
        out_shape=[jax.ShapeDtypeStruct((depth + part // 2, 2 * width), BF16)] * 2,
        in_specs=[pl.BlockSpec(memory_space=pltpu.SMEM)] + [anywhere] * 3 + [vmem],
        out_specs=[vmem] * 2,
        scratch_shapes=[
            pltpu.VMEM((2, 2, depth, width), F32),
            pltpu.VMEM((2, part, width), F32),
            pltpu.SemaphoreType.DMA((2, 3)),
        ],
        cost_estimate=pl.CostEstimate(
            flops=4 * depth * width, bytes_accessed=24 * depth * width, transcendentals=0
        ),
    )(at, value, gate, pool, scales)


def mixer_kernel(which, depth, rows, tile, idx, x_hbm, *refs):
    out, xv, wv, acc, pv, sem = refs[-6:]
    blocks = (len(refs) - 6) // 2
    halves = refs[:blocks], refs[blocks : 2 * blocks]
    width = out.shape[1]
    half = width // 2
    lines = wv.shape[1] - depth

    copies = []
    for k in range(blocks):
        cols = pl.ds(pl.multiple_of(idx[k] * depth, depth), depth)
        copies.append(
            [
                pltpu.make_async_copy(
                    halves[j][k], wv.at[k, :, j * width : (j + 1) * width], sem.at[j, k]
                )
                for j in range(2)
            ]
            + [pltpu.make_async_copy(x_hbm.at[:, cols], xv.at[k], sem.at[2, k])]
        )
    for group in copies:
        for copy in group:
            copy.start()
    window, member = idx[blocks + which], idx[blocks + 2]
    for early in (True, False):
        ks = range(blocks // 2) if early else range(blocks // 2, blocks)
        for k in ks:
            for copy in copies[k]:
                copy.wait()

        def product(m, carry, ks=ks, early=early):
            at = pl.ds(pl.multiple_of(m * tile, tile), tile)
            total = dot(xv[ks[0], at, :], wv[ks[0], :depth, :])
            for k in ks[1:]:
                total = total + dot(xv[k, at, :], wv[k, :depth, :])
            acc[at, :] = total if early else acc[at, :] + total
            return carry

        lax.fori_loop(0, rows // tile, product, 0)
    for k in range(blocks):
        base = pl.multiple_of(idx[k] * 2 * lines + member * half, 2 * lines)
        base = jnp.where(base >= width, base - width, base)
        for j in range(2):
            for part in range(2):
                at = pl.ds(pl.multiple_of(base + part * lines, lines), lines)
                cols = slice(j * width + part * half, j * width + (part + 1) * half)
                pv[at, j * half : (j + 1) * half] = wv[k, depth:, cols]

    def columns(at, first):
        return jnp.concatenate([acc[at, pl.ds(j * width + first, half)] for j in range(2)], axis=1)

    t = lax.broadcasted_iota(jnp.int32, (tile, tile), 0)
    s = lax.broadcasted_iota(jnp.int32, (tile, tile), 1)
    here = jnp.where((s <= t) & (s > t - window), 1.0, 0.0).astype(BF16)
    back = jnp.where(s - tile > t - window, 1.0, 0.0).astype(BF16)
    before = None
    for m in range(rows // tile):
        at = pl.ds(m * tile, tile)
        value = columns(at, 0).astype(BF16)
        running = dot(here, value)
        if m:
            running = running + dot(back, before)
        before = value
        place = lax.broadcasted_iota(jnp.int32, (tile, 1), 0) + m * tile
        counts = jnp.minimum(place + 1, window).astype(F32)
        excess = (running / counts - value.astype(F32)).astype(BF16)
        pooled = dot(excess, pv[...])
        merged = (jax.nn.sigmoid(columns(at, half)) * pooled).astype(BF16)
        for j in range(2):
            who = 1 - member if j else member
            out[at, pl.ds(pl.multiple_of(who * half, half), half)] = merged[:, j * half : (j + 1) * half]


def mixer(which, idx, x, first, second, part):
    rows = x.shape[0]
    depth = first[0].shape[0] - part // 2
    width = first[0].shape[1]
    count = len(first)
    tile = 256
    anywhere = pl.BlockSpec(memory_space=pl.ANY)
    flops = 2 * rows * (count * depth * 2 * width + 2 * tile * width + width * width)
    return pl.pallas_call(
        functools.partial(mixer_kernel, which, depth, rows, tile),
        out_shape=jax.ShapeDtypeStruct((rows, width), BF16),
        in_specs=[pl.BlockSpec(memory_space=pltpu.SMEM)] + [anywhere] * (2 * count + 1),
        out_specs=pl.BlockSpec(memory_space=pltpu.VMEM),
        scratch_shapes=[
            pltpu.VMEM((count, rows, depth), BF16),
            pltpu.VMEM((count, first[0].shape[0], 2 * width), BF16),
            pltpu.VMEM((rows, 2 * width), F32),
            pltpu.VMEM((count * part, width), BF16),
            pltpu.SemaphoreType.DMA((3, count)),
        ],
        cost_estimate=pl.CostEstimate(
            flops=flops, bytes_accessed=2 * (x.size + 2 * count * first[0].size), transcendentals=0
        ),
        compiler_params=pltpu.CompilerParams(vmem_limit_bytes=32 * 2**20),
    )(idx, x, *first, *second)


def up_kernel(own, kept, idx, gain, tokens, m0, m1, m2, m3, *refs):
    count = (len(refs) - (9 if own else 8)) // 2
    blocks, refs = refs[: 2 * count], refs[2 * count :]
    if own:
        first, second, middle, tok, parts, wide, normed, wv, sem = refs
    else:
        first, second, tok, parts, wide, normed, wv, sem = refs
    model = tok.shape[1]
    depth, width = blocks[0].shape
    group = m0.shape[1]
    member = idx[count + 2]
    who = member if own else 1 - member
    at = pl.ds(pl.multiple_of(who * kept, kept), kept)
    copies = [pltpu.make_async_copy(tokens.at[at, :], tok, sem.at[0])]
    for k, part in enumerate((m0, m1, m2, m3)):
        copies.append(pltpu.make_async_copy(part.at[at, :], parts.at[k], sem.at[1 + k]))
    weights = [
        pltpu.make_async_copy(
            b, wv.at[k // count, pl.ds((k % count) * depth, depth), :], sem.at[5 + k]
        )
        for k, b in enumerate(blocks)
    ]
    for copy in copies + weights:
        copy.start()
    for copy in copies:
        copy.wait()
    total = jnp.zeros((kept, 1), F32)
    for k in range(4):
        cols = pl.ds(pl.multiple_of(idx[count + 3 + k] * group, group), group)
        values = tok[:, cols].astype(F32) + parts[k].astype(F32)
        wide[:, cols] = values
        total = total + jnp.sum(values * values, axis=1, keepdims=True)
    scale = lax.rsqrt(total / model + EPS)
    for k in range(count):
        cols = pl.ds(pl.multiple_of(idx[k] * depth, depth), depth)
        normed[:, k * depth : (k + 1) * depth] = (wide[:, cols] * scale * gain[:, cols]).astype(BF16)
    step = 512 if width % 512 == 0 else width
    for j, out in enumerate((first, second)):
        for copy in weights[j * count : (j + 1) * count]:
            copy.wait()

        def product(n, carry, out=out, j=j):
            cols = pl.ds(pl.multiple_of(n * step, step), step)
            up = jnp.maximum(dot(normed[...], wv[j, :, cols]), 0.0)
            out[:, cols] = (up * up).astype(BF16)
            return carry

        lax.fori_loop(0, width // step, product, 0)
    if own:
        middle[...] = wide[...]


def upward(own, idx, tokens, parts, gain, mine, theirs, kept):
    _, model = tokens.shape
    depth, width = mine[0].shape
    count = len(mine)
    anywhere = pl.BlockSpec(memory_space=pl.ANY)
    smem, vmem = pl.BlockSpec(memory_space=pltpu.SMEM), pl.BlockSpec(memory_space=pltpu.VMEM)
    hidden = jax.ShapeDtypeStruct((kept, width), BF16)
    more = [jax.ShapeDtypeStruct((kept, model), F32)] if own else []
    return pl.pallas_call(
        functools.partial(up_kernel, own, kept),
        out_shape=[hidden, hidden] + more,
        in_specs=[smem, vmem] + [anywhere] * (5 + 2 * count),
        out_specs=[vmem] * (2 + len(more)),
        scratch_shapes=[
            pltpu.VMEM((kept, model), BF16),
            pltpu.VMEM((4, kept, parts[0].shape[1]), BF16),
            pltpu.VMEM((kept, model), F32),
            pltpu.VMEM((kept, model), BF16),
            pltpu.VMEM((2, count * depth, width), BF16),
            pltpu.SemaphoreType.DMA((5 + 2 * count,)),
        ],
        cost_estimate=pl.CostEstimate(
            flops=4 * kept * model * width,
            bytes_accessed=2 * (2 * kept * model + 2 * model * width),
            transcendentals=0,
        ),
        compiler_params=pltpu.CompilerParams(vmem_limit_bytes=32 * 2**20),
    )(idx, gain.reshape(1, model), tokens, *parts, *mine, *theirs)


def down_kernel(h0, h1, *refs):
    out = refs[-1]
    count = (len(refs) - 1) // 2
    width = refs[0].shape[1]
    for k in range(count):
        total = dot(h0[...], refs[k][...]) + dot(h1[...], refs[count + k][...])
        out[:, k * width : (k + 1) * width] = total.astype(BF16)


def down(h0, h1, own, other):
    count = len(own)
    rows, width = h0.shape[0], own[0].shape[1]
    vmem = pl.BlockSpec(memory_space=pltpu.VMEM)
    return pl.pallas_call(
        down_kernel,
        out_shape=jax.ShapeDtypeStruct((rows, count * width), BF16),
        in_specs=[vmem] * (2 + 2 * count),
        out_specs=vmem,
        cost_estimate=pl.CostEstimate(
            flops=4 * h0.size * count * width,
            bytes_accessed=4 * (h0.size + count * own[0].size),
            transcendentals=0,
        ),
        compiler_params=pltpu.CompilerParams(vmem_limit_bytes=16 * 2**20),
    )(h0, h1, *own, *other)


def final_kernel(sequence, idx, middle, *refs):
    out, base, done, sem = refs[-4:]
    count = len(sequence)
    keeps, gots = refs[:count], refs[count:-4]
    group = len(sequence[0])
    width = keeps[0].shape[1] // group
    copies = []
    for j in range(count):
        for k in range(group):
            part = slice(k * width, (k + 1) * width)
            cols = pl.ds(pl.multiple_of(idx[sequence[j][k]] * width, width), width)
            summed = middle[:, cols] + keeps[j][:, part].astype(F32)
            if j == count - 1:
                base[:, part] = summed
            else:
                i = j * group + k
                done[i] = (summed + gots[j][:, part].astype(F32)).astype(BF16)
                copies.append(pltpu.make_async_copy(done.at[i], out.at[:, cols], sem.at[i]))
                copies[-1].start()
    for copy in copies:
        copy.wait()


def final(sequence, idx, middle, keeps, gots):
    kept, model = middle.shape
    wide = keeps[0].shape[1]
    group, count = len(sequence[0]), len(keeps)
    vmem = pl.BlockSpec(memory_space=pltpu.VMEM)
    moved = (count - 1) * group
    return pl.pallas_call(
        functools.partial(final_kernel, sequence),
        out_shape=[
            jax.ShapeDtypeStruct((kept, model), BF16),
            jax.ShapeDtypeStruct((kept, wide), F32),
        ],
        in_specs=[pl.BlockSpec(memory_space=pltpu.SMEM)] + [vmem] * (1 + 2 * count - 1),
        out_specs=[pl.BlockSpec(memory_space=pl.ANY), vmem],
        scratch_shapes=[
            pltpu.VMEM((moved, kept, wide // group), BF16),
            pltpu.SemaphoreType.DMA((moved,)),
        ],
        cost_estimate=pl.CostEstimate(
            flops=2 * kept * model, bytes_accessed=10 * kept * model, transcendentals=0
        ),
        compiler_params=pltpu.CompilerParams(vmem_limit_bytes=16 * 2**20),
    )(idx, middle, *keeps, *gots)


def finish_kernel(last, idx, base, got, before, out, done, sem):
    del before
    width = done.shape[2]
    copies = []
    for k, place in enumerate(last):
        part = slice(k * width, (k + 1) * width)
        cols = pl.ds(pl.multiple_of(idx[place] * width, width), width)
        done[k] = (base[:, part] + got[:, part].astype(F32)).astype(BF16)
        copies.append(pltpu.make_async_copy(done.at[k], out.at[:, cols], sem.at[k]))
        copies[-1].start()
    for copy in copies:
        copy.wait()


def finish(last, idx, base, got, before):
    kept, wide = base.shape
    vmem, anywhere = pl.BlockSpec(memory_space=pltpu.VMEM), pl.BlockSpec(memory_space=pl.ANY)
    return pl.pallas_call(
        functools.partial(finish_kernel, last),
        out_shape=jax.ShapeDtypeStruct(before.shape, BF16),
        in_specs=[pl.BlockSpec(memory_space=pltpu.SMEM), vmem, vmem, anywhere],
        out_specs=anywhere,
        scratch_shapes=[
            pltpu.VMEM((len(last), kept, wide // len(last)), BF16),
            pltpu.SemaphoreType.DMA((len(last),)),
        ],
        input_output_aliases={3: 0},
        cost_estimate=pl.CostEstimate(
            flops=2 * kept * wide, bytes_accessed=10 * kept * wide, transcendentals=0
        ),
        compiler_params=pltpu.CompilerParams(vmem_limit_bytes=8 * 2**20),
    )(idx, base, got, before)


def paired(
    tokens,
    mixer_gain,
    value_weight,
    value_scale,
    gate_weight,
    gate_scale,
    pool_weight,
    pool_scale,
    channel_gain,
    up_weight,
    up_scale,
    down_weight,
    down_scale,
):
    _, rows, model = tokens.shape
    tokens = tokens.reshape(rows, model)
    fs = lax.axis_size("fs")
    line = fs // 2
    t, r, f = lax.axis_index("tp"), lax.axis_index("rep"), lax.axis_index("fs")
    kept = rows // 2
    part = pool_weight.shape[1]

    order = ring_order(line)
    place = {z: p for p, z in enumerate(order)}
    swap = [(0, 1), (1, 0)]
    side = [(z * 2 + y, z * 2 + 1 - y) for z in range(line) for y in range(2)]
    step = [
        (z * 2 + y, order[(place[z] + 1) % line] * 2 + y) for z in range(line) for y in range(2)
    ]

    across = lambda v: lax.ppermute(v, "tp", swap)
    core = lambda v: lax.ppermute(v, "rep", swap)
    beside = lambda v: lax.ppermute(v, "fs", side)
    onward = lambda v: lax.ppermute(v, "fs", step)

    def facts(z, y, t, r):
        at = [order[(place[z] - k) % line] * 2 for k in range(line)]
        groups = [2 * t + r, 2 * t + 1 - r, 2 * (1 - t) + r, 2 * (1 - t) + 1 - r]
        windows = [2 ** (g + 1) for g in groups[:2]]
        return [b + y for b in at] + [b + 1 - y for b in at] + windows + [t] + groups

    table = np.array(
        [
            facts(z, y, tt, rr)
            for z in range(line)
            for y in range(2)
            for tt in range(2)
            for rr in range(2)
        ],
        np.int32,
    )
    idx = lax.dynamic_index_in_dim(jnp.asarray(table), (f * 2 + t) * 2 + r, 0, keepdims=False)

    def gathered(block, by_side):
        own, other = [block], []
        for k in range(line):
            if k < line - 1 or by_side:
                other.append(beside(own[k]))
            else:
                other.append(onward(other[k - 1]))
            if k < line - 1:
                own.append(onward(own[k]))
        blocks = own + other
        return blocks, [core(b) for b in blocks]

    scales = jnp.stack([value_scale, gate_scale, pool_scale])
    mix_block, mix_send = prepare(
        jnp.stack([idx[fs + 3], idx[fs + 5]]), value_weight, gate_weight, pool_weight, scales
    )
    mix_got = across(mix_send)

    up_width = up_weight.shape[1] // 2
    up_own = lax.dynamic_slice_in_dim(up_weight, r * up_width, up_width, 1)
    up_block = (up_own * lax.dynamic_slice_in_dim(up_scale, r * up_width, up_width, 0)).astype(BF16)
    down_depth = down_weight.shape[0] // 2
    down_block = lax.dynamic_slice_in_dim(down_weight, r * down_depth, down_depth, 0)
    down_block = (down_block * down_scale).astype(BF16)

    first_own, first_other = gathered(mix_block, False)
    second_own, second_other = gathered(mix_got, True)
    up_mine, up_theirs = gathered(up_block, True)
    down_mine, down_theirs = gathered(down_block, False)

    normed = norm_rows(tokens, mixer_gain).astype(BF16)

    merged_own = mixer(0, idx, normed, first_own, second_own, part)
    from_own = across(merged_own)
    merged_other = mixer(1, idx, normed, first_other, second_other, part)
    from_other = across(merged_other)

    parts = (merged_own, merged_other, from_own, from_other)
    sent_own, sent_other = upward(False, idx, tokens, parts, channel_gain, up_mine, up_theirs, kept)
    kept_own, kept_other, middle = upward(
        True, idx, tokens, parts, channel_gain, up_mine, up_theirs, kept
    )

    sequence = [(0, 1)] + [(line + k, k + 1) for k in range(1, line - 1)] + [(line, fs - 1)]
    keeps, gots = [], []
    for which in sequence:
        mine_k, theirs_k = [[a[i] for i in which] for a in (down_mine, down_theirs)]
        send = down(sent_own, sent_other, mine_k, theirs_k)
        gots.append(across(send))
        keeps.append(down(kept_own, kept_other, mine_k, theirs_k))
    out, base = final(sequence, idx, middle, keeps, gots[:-1])
    out = finish(sequence[-1], idx, base, gots[-1], out)
    return out.reshape(1, kept, model)


def solution(mesh):
    sizes = dict(mesh.shape)

    def per_device(tokens, mixer_gain, value_weight, value_scale, *rest):
        fits = (
            sizes["rep"] == 2
            and sizes["tp"] == 2
            and sizes["fs"] % 4 == 0
            and tokens.shape[0] == 1
            and value_scale.shape[0] == 4
            and value_weight.shape[0] % 128 == 0
            and value_weight.shape[2] % 128 == 0
            and rest[2].shape[1] % 32 == 0
            and tokens.shape[1] % 256 == 0
        )
        return (paired if fits else general)(tokens, mixer_gain, value_weight, value_scale, *rest)

    return jax.shard_map(
        per_device,
        mesh=mesh,
        in_specs=(
            P(("rep", "fs"), None, None),
            P(),
            P("fs", None, "tp"),
            P(None, "tp"),
            P("fs", None, "tp"),
            P(None, "tp"),
            P(None, "fs", "tp"),
            P(None, "tp"),
            P(),
            P("fs", "tp"),
            P("tp"),
            P("tp", "fs"),
            P("fs"),
        ),
        out_specs=P(("rep", "fs"), "tp", None),
        check_vma=False,
    )
```
